32 devices in a mesh: sp: 16 (over z, y, core), tp: 2 (over x).
Axes of the slice: x: 2, y: 2, z: 4, core: 2. Of those that a mesh axis runs over, the one named last changes fastest.
Arguments:
- queries: bfloat16 [4096, 512], P('sp', 'tp'), may hold values from -8 to 8
- keys: bfloat16 [4096, 512], P('sp', 'tp'), may hold values from -8 to 8
- values: bfloat16 [4096, 512], P('sp', 'tp'), may hold values from -6 to 6
- score_shift: float32 [8], P('tp'), may hold values from 3 to 20
- resid: bfloat16 [4096, 2048], P(('sp', 'tp')), may hold values from -6 to 6
- w_out: bfloat16 [512, 2048], replicated, may hold values from -0.25 to 0.25
- gain_mix: float32 [2048], replicated, may hold values from 0.1 to 1.9
- gain_pre: float32 [2048], replicated, may hold values from 0.1 to 1.9
- w_gate: bfloat16 [2048, 5632], P('sp', 'tp'), may hold values from -0.125 to 0.125
- w_up: bfloat16 [2048, 5632], P('sp', 'tp'), may hold values from -0.125 to 0.125
- conv_gate: float32 [3, 5632], P(None, 'tp'), may hold values from -3 to 3
- conv_up: float32 [3, 5632], P(None, 'tp'), may hold values from -3 to 3
- w_down: bfloat16 [5632, 2048], P('tp', 'sp'), may hold values from -0.078125 to 0.078125
- gain_post: float32 [2048], replicated, may hold values from 0.1 to 1.9
Outputs:
- result: bfloat16 [4096, 2048], P(('sp', 'tp'))
The draws below stay inside these ranges and needn't reach their ends.
All inputs are finite; a program needn't handle non-finite values.
Results may differ from the reference program's by a relative error of at most 0.017.
Values may be sent and summed in bfloat16 or wider, within the bound.
No kernel may reach another device: no remote copies, remote signals or barrier semaphores. Data moves between devices by JAX's collectives and lax.ppermute only.
A program may use at most 128 MiB of HBM per device.

```python
import math
import jax
import jax.numpy as jnp
from jax import lax

D = 2048
HEADS = 8
HEAD_DIM = 64
FF = 5632
KERNEL = 3
SEQ = 4096
N_TP = 2


def level_of(rng, dims, split, low, top_value):
    gain, own = 1.0, jax.random.fold_in(rng, 6)
    for axis_at, parts in split:
        heights = jnp.exp(jax.random.uniform(jax.random.fold_in(own, axis_at), (parts,), jnp.float32, low / len(split), top_value / len(split)))
        gain = gain * jnp.repeat(heights, dims[axis_at] // parts).reshape([-1 if axis == axis_at else 1 for axis in range(len(dims))])
    return gain


def scatter_about(key, dims, deviation, limit, shards=(), kind=jnp.bfloat16):
    factor_of = level_of(key, dims, shards, -0.22, 0.18) if shards else 1.0
    values = jax.random.normal(key, dims, jnp.float32) * deviation * factor_of
    return jnp.minimum(jnp.maximum(values, -limit), limit).astype(kind)


def setup_inputs(seed: int = 0) -> dict:
    arg_keys = jax.random.split(jax.random.key(seed), 15)
    queries = scatter_about(arg_keys[0], (SEQ, HEADS * HEAD_DIM), 2.0, 8.0, ((0, 16), (1, 2)))
    keys = scatter_about(arg_keys[1], (SEQ, HEADS * HEAD_DIM), 2.0, 8.0, ((0, 16), (1, 2)))
    values = scatter_about(arg_keys[2], (SEQ, HEADS * HEAD_DIM), 1.0, 6.0, ((0, 16), (1, 2)))
    score_shift = jnp.clip(jnp.exp(math.log(20.0) - 1.89712 * jax.random.uniform(arg_keys[3], (HEADS,), jnp.float32) ** level_of(arg_keys[3], (HEADS,), ((0, 2),), -0.2, 0.2)), 3.0, 20.0)
    resid = scatter_about(arg_keys[4], (SEQ, D), 1.0, 6.0, ((0, 32),))
    w_out = scatter_about(arg_keys[5], (HEADS * HEAD_DIM, D), (HEADS * HEAD_DIM) ** -0.5, 0.25)
    gain_mix = jnp.clip(1.0 + 0.18 * jax.random.normal(arg_keys[6], (D,), jnp.float32), 0.1, 1.9)
    gain_pre = jnp.clip(1.0 + 0.18 * jax.random.normal(arg_keys[7], (D,), jnp.float32), 0.1, 1.9)
    w_gate = scatter_about(arg_keys[8], (D, FF), D ** -0.5, 0.125, ((0, 16), (1, 2)))
    w_up = scatter_about(arg_keys[9], (D, FF), D ** -0.5, 0.125, ((0, 16), (1, 2)))
    conv_gate = scatter_about(arg_keys[10], (KERNEL, FF), 0.577, 3.0, ((1, 2),), jnp.float32)
    conv_up = scatter_about(arg_keys[11], (KERNEL, FF), 0.577, 3.0, ((1, 2),), jnp.float32)
    w_down = scatter_about(arg_keys[12], (FF, D), FF ** -0.5, 0.078125, ((0, 2), (1, 16)))
    gain_post = jnp.clip(1.0 + 0.18 * jax.random.normal(arg_keys[13], (D,), jnp.float32), 0.1, 1.9)
    return dict(queries=queries, keys=keys, values=values, score_shift=score_shift, resid=resid, w_out=w_out, gain_mix=gain_mix, gain_pre=gain_pre, w_gate=w_gate, w_up=w_up, conv_gate=conv_gate, conv_up=conv_up, w_down=w_down, gain_post=gain_post)


def rms_scale(values_in):
    return values_in * lax.rsqrt(lax.optimization_barrier(jnp.mean(values_in * values_in, axis=-1, keepdims=True)) + 1e-06)

def stick_attention(queries, keys, values, score_shift):
    length = queries.shape[0]
    query_heads = queries.reshape(length, HEADS, HEAD_DIM).transpose(1, 0, 2)
    key_heads = keys.reshape(length, HEADS, HEAD_DIM).transpose(1, 0, 2)
    value_heads = values.reshape(length, HEADS, HEAD_DIM).transpose(1, 0, 2)
    block = math.gcd(length, 512)
    blocks = length // block
    key_pos = jnp.arange(length, dtype=jnp.int32)

    def one_block(index):
        head = index // blocks
        first = index % blocks * block
        query_block = lax.dynamic_slice(query_heads, (head, first, jnp.int32(0)), (1, block, HEAD_DIM))[0]
        key_head = lax.dynamic_index_in_dim(key_heads, head, 0, keepdims=False)
        value_head = lax.dynamic_index_in_dim(value_heads, head, 0, keepdims=False)
        shift = lax.dynamic_index_in_dim(score_shift, head, 0, keepdims=False)
        scores = jnp.dot(query_block, key_head.T, preferred_element_type=jnp.float32) * HEAD_DIM ** (-0.5) - shift
        query_pos = first + jnp.arange(block, dtype=jnp.int32)
        causal = key_pos[None, :] < query_pos[:, None]
        log_keep = jnp.where(causal, -jax.nn.softplus(scores), 0.0)
        later = lax.cumsum(log_keep, axis=1, reverse=True) - log_keep
        weights = jnp.where(causal, jnp.exp(jax.nn.log_sigmoid(scores) + later), 0.0).astype(jnp.bfloat16)
        return jnp.dot(weights, value_head, preferred_element_type=jnp.float32).astype(jnp.bfloat16)
    outputs = lax.map(one_block, jnp.arange(HEADS * blocks, dtype=jnp.int32))
    outputs = outputs.reshape(HEADS, length, HEAD_DIM)
    return outputs.transpose(1, 0, 2).reshape(length, HEADS * HEAD_DIM)

def reference(queries, keys, values, score_shift, resid, w_out, gain_mix, gain_pre, w_gate, w_up, conv_gate, conv_up, w_down, gain_post):
    attended = stick_attention(queries, keys, values, score_shift)
    mixed = jnp.dot(attended, w_out, preferred_element_type=jnp.float32).astype(jnp.bfloat16)
    middle = (resid.astype(jnp.float32) + gain_mix * rms_scale(mixed.astype(jnp.float32))).astype(jnp.bfloat16)
    normed = (gain_pre * rms_scale(middle.astype(jnp.float32))).astype(jnp.bfloat16)
    gate_proj = jnp.dot(normed, w_gate, preferred_element_type=jnp.float32).astype(jnp.bfloat16)
    up_proj = jnp.dot(normed, w_up, preferred_element_type=jnp.float32).astype(jnp.bfloat16)
    length = normed.shape[0]
    gate_pad = jnp.pad(gate_proj.astype(jnp.float32), ((KERNEL - 1, 0), (0, 0)))
    up_pad = jnp.pad(up_proj.astype(jnp.float32), ((KERNEL - 1, 0), (0, 0)))
    gate_conv = jnp.zeros((length, FF), jnp.float32)
    up_conv = jnp.zeros((length, FF), jnp.float32)
    for tap in range(KERNEL):
        gate_conv = gate_conv + conv_gate[tap] * gate_pad[tap:tap + length]
        up_conv = up_conv + conv_up[tap] * up_pad[tap:tap + length]
    hidden = (jax.nn.silu(gate_conv) * up_conv).astype(jnp.bfloat16)
    width_block = FF // N_TP
    summed = jnp.zeros((length, D), jnp.float32)
    for index in range(N_TP):
        partial_sum = jnp.dot(hidden[:, index * width_block:(index + 1) * width_block], w_down[index * width_block:(index + 1) * width_block], preferred_element_type=jnp.float32)
        summed = summed + partial_sum.astype(jnp.bfloat16).astype(jnp.float32)
    ffn_out = summed.astype(jnp.bfloat16)
    return (middle.astype(jnp.float32) + gain_post * rms_scale(ffn_out.astype(jnp.float32))).astype(jnp.bfloat16)
```

```python
import functools
import math

import jax
import jax.numpy as jnp
from jax import lax
from jax.experimental import pallas as pl
from jax.experimental.pallas import tpu as pltpu
from jax.sharding import PartitionSpec as P

HEAD_DIM = 64
KERNEL = 3
HALO = 16
LANES = 128
EPS = 1e-06
LOG2E = math.log2(math.e)
AXES = ("sp", "tp")


def from_behind(x, axis, by):
    length = lax.axis_size(axis)
    pairs = [(i, i + by) for i in range(length) if 0 <= i + by < length]
    return lax.ppermute(x, axis, pairs)


def rms_scale(values_in):
    return values_in * lax.rsqrt(jnp.mean(values_in * values_in, axis=-1, keepdims=True) + EPS)


def plain_attention(queries, key_whole, value_whole, score_shift):
    tok_rows = queries.shape[0]
    local_heads = queries.shape[1] // HEAD_DIM
    total = key_whole.shape[0]
    shards = total // tok_rows
    group = max(
        factor
        for factor in range(1, shards + 1)
        if shards % factor == 0 and factor * tok_rows <= max(2048, tok_rows)
    )
    span = group * tok_rows
    offset = lax.axis_index("sp") * tok_rows
    query_heads = queries.reshape(tok_rows, local_heads, HEAD_DIM)
    key_heads = key_whole.reshape(total, local_heads, HEAD_DIM)
    value_heads = value_whole.reshape(total, local_heads, HEAD_DIM)
    query_pos = offset + jnp.arange(tok_rows, dtype=jnp.int32)
    last_block = (offset + tok_rows - 1) // span

    def visit(turn, carry):
        accum, tail = carry
        block_start = (last_block - turn) * span
        key_block = lax.dynamic_slice_in_dim(key_heads, block_start, span, 0)
        value_block = lax.dynamic_slice_in_dim(value_heads, block_start, span, 0)
        scores = jnp.einsum(
            "qhd,khd->hqk", query_heads, key_block, preferred_element_type=jnp.float32
        )
        scores = scores * HEAD_DIM ** (-0.5) - score_shift[:, None, None]
        key_pos = block_start + jnp.arange(span, dtype=jnp.int32)
        causal = (key_pos[None, :] < query_pos[:, None])[None, :, :]
        log_keep = jnp.where(causal, -jax.nn.softplus(scores), 0.0)
        later = lax.cumsum(log_keep, axis=2, reverse=True) - log_keep
        weights = jnp.where(
            causal, jnp.exp(jax.nn.log_sigmoid(scores) + later + tail[:, :, None]), 0.0
        ).astype(jnp.bfloat16)
        accum = accum + jnp.einsum(
            "hqk,khd->hqd", weights, value_block, preferred_element_type=jnp.float32
        )
        return (accum, tail + jnp.sum(log_keep, axis=2))

    start_carry = (
        jnp.zeros((local_heads, tok_rows, HEAD_DIM), jnp.float32),
        jnp.zeros((local_heads, tok_rows), jnp.float32),
    )
    accum, _ = lax.fori_loop(0, last_block + 1, visit, start_carry)
    return accum.transpose(1, 0, 2).reshape(tok_rows, local_heads * HEAD_DIM).astype(jnp.bfloat16)


def plain_local(
    queries, keys, values, score_shift, resid, w_out, gain_mix, gain_pre,
    w_gate, w_up, conv_gate, conv_up, w_down, gain_post,
):
    gate_whole = lax.all_gather(w_gate, "sp", axis=0, tiled=True)
    up_whole = lax.all_gather(w_up, "sp", axis=0, tiled=True)
    down_whole = lax.all_gather(w_down, "sp", axis=1, tiled=True)
    key_whole = lax.all_gather(keys, "sp", axis=0, tiled=True)
    value_whole = lax.all_gather(values, "sp", axis=0, tiled=True)
    attended = plain_attention(queries, key_whole, value_whole, score_shift)
    head_rows = lax.all_to_all(attended, "tp", split_axis=0, concat_axis=1, tiled=True)
    mixed = jnp.dot(head_rows, w_out, preferred_element_type=jnp.float32).astype(jnp.bfloat16)
    middle = (resid.astype(jnp.float32) + gain_mix * rms_scale(mixed.astype(jnp.float32))).astype(
        jnp.bfloat16
    )
    normed = (gain_pre * rms_scale(middle.astype(jnp.float32))).astype(jnp.bfloat16)
    piece = lax.all_gather(normed, "tp", axis=0, tiled=True)
    gate_part = jnp.dot(piece, gate_whole, preferred_element_type=jnp.float32).astype(jnp.bfloat16)
    up_part = jnp.dot(piece, up_whole, preferred_element_type=jnp.float32).astype(jnp.bfloat16)
    projected = jnp.concatenate([gate_part, up_part], axis=1)
    tok_rows = projected.shape[0]
    local_units = projected.shape[1] // 2
    edge = from_behind(projected[tok_rows - (KERNEL - 1) :], "sp", 1)
    extended = jnp.concatenate([edge, projected], axis=0).astype(jnp.float32)
    taps = jnp.concatenate([conv_gate, conv_up], axis=1)
    convolved = taps[0] * extended[0:tok_rows]
    for tap in range(1, KERNEL):
        convolved = convolved + taps[tap] * extended[tap : tap + tok_rows]
    hidden = (jax.nn.silu(convolved[:, :local_units]) * convolved[:, local_units:]).astype(
        jnp.bfloat16
    )
    summed = lax.psum_scatter(
        jnp.dot(hidden, down_whole, preferred_element_type=jnp.float32).astype(jnp.bfloat16),
        "tp",
        scatter_dimension=0,
        tiled=True,
    )
    return (middle.astype(jnp.float32) + gain_post * rms_scale(summed.astype(jnp.float32))).astype(
        jnp.bfloat16
    )


def attention_kernel(table, shift, q_ref, kv_ref, o_ref, acc, tail, tri):
    slots, rows, _ = q_ref.shape
    total = kv_ref.shape[0]
    per_slot = total // slots
    mine = table[total + slots]
    scale = HEAD_DIM ** (-0.5) * LOG2E
    head_shift = shift[0] * LOG2E
    row_id = lax.broadcasted_iota(jnp.int32, (rows, rows), 0)
    col_id = lax.broadcasted_iota(jnp.int32, (rows, rows), 1)
    tri[...] = jnp.where(row_id > col_id, 1.0, 0.0).astype(jnp.bfloat16)
    acc[...] = jnp.zeros_like(acc)
    tail[...] = jnp.zeros_like(tail)

    def visit(block, first, on_diagonal):
        kv = kv_ref[table[block]]
        for slot in range(first, slots):
            q = q_ref[table[total + slot]]
            raw = lax.dot_general(
                q, kv, (((1,), (1,)), ((), ())), preferred_element_type=jnp.float32
            )
            score = raw * scale - head_shift
            keep = -(jnp.maximum(score, 0.0) + jnp.log2(1.0 + jnp.exp2(-jnp.abs(score))))
            masked = on_diagonal and slot == first
            if masked:
                causal = row_id > col_id
                keep = jnp.where(causal, keep, 0.0)
            later = jnp.dot(
                keep.astype(jnp.bfloat16), tri[...], preferred_element_type=jnp.float32
            )
            rest = tail[slot]
            weight = jnp.exp2(score + keep + later + rest)
            if masked:
                weight = jnp.where(causal, weight, 0.0)
            tail[slot] = rest + later[:, :1] + keep[:, :1]
            acc[slot] = acc[slot] + jnp.dot(
                weight.astype(jnp.bfloat16), kv, preferred_element_type=jnp.float32
            )

    for first in range(slots - 1, -1, -1):
        top = per_slot * first + mine
        visit(top, first, True)

        def step(turn, _, top=top, first=first):
            visit(top - turn, first, False)
            return 0

        lax.fori_loop(1, per_slot if first else mine + 1, step, 0)
    half = slots // 2
    for slot in range(half):
        o_ref[slot] = jnp.concatenate(
            [acc[slot][:, HEAD_DIM:], acc[slot + half][:, HEAD_DIM:]], axis=1
        ).astype(o_ref.dtype)


def mix_kernel(
    table, att_ref, w_ref, resid_ref, gain_mix, gain_pre, normed_ref, middle_ref, edge_ref, w_perm
):
    heads = w_ref.shape[0]
    chunks = normed_ref.shape[2] // LANES
    half_rows = resid_ref.shape[1]
    z, x, h_mine = table[chunks], table[chunks + 1], table[chunks + 2]
    per = heads // 2
    for piece in range(heads):
        head = (x ^ (piece // per)) * per + (z ^ (piece % per))
        w_perm[piece * HEAD_DIM : (piece + 1) * HEAD_DIM, :] = w_ref[head]
    for tile in range(4):
        h = h_mine ^ (tile // 2)
        row = pl.multiple_of((x ^ (tile % 2)) * half_rows, half_rows)
        parts = []
        for piece in range(heads):
            both = att_ref[piece // per, piece % per, pl.ds(row, half_rows), :].astype(jnp.float32)
            parts.append(jnp.where(h == 0, both[:, :HEAD_DIM], both[:, HEAD_DIM:]))
        att = jnp.concatenate(parts, axis=1).astype(jnp.bfloat16)
        mixed = jnp.dot(att, w_perm[...], preferred_element_type=jnp.float32)
        mixed = mixed.astype(jnp.bfloat16).astype(jnp.float32)
        scaled = mixed * lax.rsqrt(jnp.mean(mixed * mixed, axis=-1, keepdims=True) + EPS)
        middle = (resid_ref[tile].astype(jnp.float32) + gain_mix[...] * scaled).astype(jnp.bfloat16)
        if tile == 0:
            middle_ref[...] = middle
        wide = middle.astype(jnp.float32)
        normed = wide * lax.rsqrt(jnp.mean(wide * wide, axis=-1, keepdims=True) + EPS)
        normed = (gain_pre[...] * normed).astype(jnp.bfloat16)

        @pl.when(row > 0)
        def _(h=h, normed=normed):
            edge_ref[h] = normed[half_rows - HALO :]

        for chunk in range(chunks):
            column = pl.multiple_of(table[chunk] * LANES, LANES)
            normed_ref[h, pl.ds(row, half_rows), pl.ds(column, LANES)] = normed[
                :, chunk * LANES : (chunk + 1) * LANES
            ]


def ffn_kernel(tiles, groups, table, normed_ref, edge_ref, *refs):
    gu_refs = refs[:groups]
    dn_refs = refs[groups : 2 * groups]
    taps_ref = refs[2 * groups]
    outs = refs[2 * groups + 1 : 2 * groups + 5]
    extended, hidden, wide = refs[2 * groups + 5 :]
    step = pl.program_id(0)
    _, rows, width = normed_ref.shape
    chunks = width // LANES
    x, h_mine, first = table[chunks + 1], table[chunks + 2], table[chunks + 3]
    ext = rows + HALO
    half_rows = rows // 2
    depth = width // groups

    @pl.when(step == 0)
    def _():
        for h in range(2):
            extended[h * ext + HALO : (h + 1) * ext, :] = normed_ref[h]
            other = edge_ref[max(h - 1, 0)]
            other = other if h else jnp.zeros_like(other)
            edge = jnp.where(first == 1, other.astype(jnp.float32), edge_ref[h].astype(jnp.float32))
            edge = edge.astype(jnp.bfloat16)
            for chunk in range(chunks):
                column = pl.multiple_of(table[chunk] * LANES, LANES)
                extended[h * ext : h * ext + HALO, pl.ds(column, LANES)] = edge[
                    :, chunk * LANES : (chunk + 1) * LANES
                ]

    @pl.when(step < tiles)
    def _():
        total = jnp.zeros((2 * ext, 2 * LANES), jnp.float32)
        for group in range(groups):
            total = total + jnp.dot(
                extended[:, group * depth : (group + 1) * depth],
                gu_refs[group][...],
                preferred_element_type=jnp.float32,
            )
        wide[...] = total
        taps = taps_ref[0]
        for tile in range(4):
            h = h_mine ^ (tile // 2)
            base = pl.multiple_of(h * ext + (x ^ (tile % 2)) * half_rows, HALO)
            window = wide[pl.ds(base, half_rows + HALO), :]
            conv = jnp.zeros((half_rows, 2 * LANES), jnp.float32)
            for tap in range(KERNEL):
                lead = HALO - (KERNEL - 1) + tap
                conv = conv + taps[tap : tap + 1, :] * window[lead : lead + half_rows, :]
            gate, up = conv[:, :LANES], conv[:, LANES:]
            act = gate / (1.0 + jnp.exp(-gate)) * up
            column = pl.multiple_of(step * LANES, LANES)
            hidden[tile * half_rows : (tile + 1) * half_rows, pl.ds(column, LANES)] = act.astype(
                jnp.bfloat16
            )

    for group in range(groups):

        @pl.when(step == tiles + group)
        def _(group=group):
            total = lax.dot_general(
                hidden[...], dn_refs[group][...], (((1,), (1,)), ((), ())),
                preferred_element_type=jnp.float32,
            )
            for tile in range(4):
                outs[tile][...] = total[tile * half_rows : (tile + 1) * half_rows].astype(
                    jnp.bfloat16
                )


def final_kernel(table, keep_ref, near_ref, far_ref, middle_ref, gain_ref, o_ref, scaled):
    rows, width = keep_ref.shape
    chunks = width // LANES
    half = width // 2
    near = keep_ref[...].astype(jnp.float32) + near_ref[...].astype(jnp.float32)
    far = far_ref[...].astype(jnp.float32)
    far = jnp.concatenate([far[:, half:], far[:, :half]], axis=1)
    out = (near + far).astype(jnp.bfloat16).astype(jnp.float32)
    scaled[...] = out * lax.rsqrt(jnp.mean(out * out, axis=-1, keepdims=True) + EPS)
    for chunk in range(chunks):
        place = pl.multiple_of(table[chunk] * LANES, LANES)
        cut = slice(chunk * LANES, (chunk + 1) * LANES)
        o_ref[:, cut] = (
            middle_ref[:, cut].astype(jnp.float32)
            + gain_ref[:, cut] * scaled[:, pl.ds(place, LANES)]
        ).astype(jnp.bfloat16)


VMEM = pl.BlockSpec(memory_space=pltpu.VMEM)
SMEM = pl.BlockSpec(memory_space=pltpu.SMEM)


def split_local(
    sp_size, tp_size, queries, keys, values, score_shift, resid, w_out, gain_mix, gain_pre,
    w_gate, w_up, conv_gate, conv_up, w_down, gain_post,
):
    rows = queries.shape[0]
    heads = queries.shape[1] // HEAD_DIM
    inner = sp_size // heads
    lane_size = sp_size // 2
    width = resid.shape[1]
    sp, x = lax.axis_index("sp"), lax.axis_index("tp")
    z, j = sp // inner, sp % inner
    h_mine, m = sp // lane_size, sp % lane_size

    def over_sp(value, flip):
        pairs = [
            (s * tp_size + t, (s ^ flip) * tp_size + t)
            for s in range(sp_size)
            for t in range(tp_size)
        ]
        return lax.ppermute(value, AXES, pairs)

    def over_tp(value):
        pairs = [
            (s * tp_size + t, s * tp_size + (t ^ 1)) for s in range(sp_size) for t in range(tp_size)
        ]
        return lax.ppermute(value, AXES, pairs)

    pick = functools.partial(lax.dynamic_index_in_dim, axis=0, keepdims=False)

    zeros = jnp.zeros((rows, HEAD_DIM), jnp.bfloat16)
    packs = []
    for head in range(heads):
        cut = slice(head * HEAD_DIM, (head + 1) * HEAD_DIM)
        packs.append(
            jnp.concatenate([queries[:, cut], zeros, keys[:, cut], values[:, cut]], axis=1)
        )
    packs = jnp.stack(packs)
    pieces = [pick(packs, z)]
    for flip in range(1, heads):
        pieces.append(over_sp(pick(packs, z ^ flip), flip * inner))
    pieces = jnp.stack(pieces)
    q_all = pieces[:, :, : 2 * HEAD_DIM]
    kv = pieces[:, :, 2 * HEAD_DIM :]
    flip = inner // 2
    order = [0]
    while flip:
        kv = jnp.concatenate([kv, over_sp(kv, flip)], axis=0)
        order = order + [o + flip for o in order]
        flip //= 2
    place = [0] * inner
    for at, o in enumerate(order):
        place[o] = at
    block_id = jnp.arange(sp_size, dtype=jnp.int32)
    flip_j = (block_id % inner) ^ j
    at_j = jnp.zeros_like(flip_j)
    for o in range(inner):
        at_j = jnp.where(flip_j == o, place[o], at_j)
    kv_table = at_j * heads + ((block_id // inner) ^ z)
    q_table = jnp.arange(heads, dtype=jnp.int32) ^ z
    table = jnp.concatenate([kv_table, q_table, j[None]]).astype(jnp.int32)
    attended = pl.pallas_call(
        attention_kernel,
        out_shape=jax.ShapeDtypeStruct((heads // 2, rows, LANES), jnp.bfloat16),
        in_specs=[SMEM, SMEM, VMEM, VMEM],
        out_specs=VMEM,
        scratch_shapes=[
            pltpu.VMEM((heads, rows, LANES), jnp.float32),
            pltpu.VMEM((heads, rows, 1), jnp.float32),
            pltpu.VMEM((rows, rows), jnp.bfloat16),
        ],
        name="attention",
    )(table, pick(score_shift, z)[None], q_all, kv)

    units = w_gate.shape[1] // 2
    tiles = units // LANES

    def weight_half(which):
        gate = lax.dynamic_slice_in_dim(w_gate, which * units, units, 1)
        up = lax.dynamic_slice_in_dim(w_up, which * units, units, 1)
        down = lax.dynamic_slice_in_dim(w_down, which * units, units, 0)
        both = jnp.stack(
            [gate.reshape(-1, tiles, LANES), up.reshape(-1, tiles, LANES)], axis=2
        ).reshape(-1, 2 * units)
        return jnp.concatenate([both, down.T], axis=1)

    kept = weight_half(h_mine)
    given = over_sp(weight_half(1 - h_mine), lane_size)
    offsets = []

    def spread(piece, base):
        flips = []
        flip = lane_size // 2
        while flip > 1:
            flips.append(flip)
            flip //= 2
        got, offs = [piece], [base]
        for f in flips:
            got = got + [over_sp(g, f) for g in got]
            offs = offs + [o ^ f for o in offs]
        first = jnp.concatenate(got, axis=0)
        offsets.extend(offs)
        offsets.extend([o ^ 1 for o in offs])
        return [first, over_sp(first, 1)]

    weights = spread(kept, 0) + spread(given, lane_size)

    half = heads // 2
    got = [pick(attended, z % half)]
    for flip in range(1, heads):
        got.append(over_sp(pick(attended, (z ^ flip) % half), flip * inner))
    got = jnp.stack(got)
    att = jnp.stack([got, over_tp(got)])
    resid_far = over_sp(resid, lane_size)
    resid_all = jnp.stack([resid, over_tp(resid), resid_far, over_tp(resid_far)])
    chunks = width // LANES
    spot = [0] * chunks
    for at, o in enumerate(offsets):
        spot[o] = at
    flip_c = jnp.arange(chunks, dtype=jnp.int32) ^ sp
    at_c = jnp.zeros_like(flip_c)
    for o in range(chunks):
        at_c = jnp.where(flip_c == o, spot[o], at_c)
    first = (m == 0).astype(jnp.int32)
    mix_table = jnp.concatenate([at_c, z[None], x[None], h_mine[None], first[None]])
    mix_table = mix_table.astype(jnp.int32)
    normed, middle, edge = pl.pallas_call(
        mix_kernel,
        out_shape=(
            jax.ShapeDtypeStruct((2, rows, width), jnp.bfloat16),
            jax.ShapeDtypeStruct(resid.shape, jnp.bfloat16),
            jax.ShapeDtypeStruct((2, HALO, width), jnp.bfloat16),
        ),
        in_specs=[SMEM, VMEM, VMEM, VMEM, VMEM, VMEM],
        out_specs=(VMEM, VMEM, VMEM),
        scratch_shapes=[pltpu.VMEM((w_out.shape[0], width), jnp.bfloat16)],
        name="mix",
    )(
        mix_table, att, w_out.reshape(-1, HEAD_DIM, width), resid_all,
        gain_mix[None], gain_pre[None],
    )

    pairs = []
    for s in range(sp_size):
        to = s // lane_size * lane_size + (s + 1) % lane_size
        pairs += [(s * tp_size + t, to * tp_size + t) for t in range(tp_size)]
    edge = lax.ppermute(edge, AXES, pairs)

    taps = jnp.stack(
        [
            lax.dynamic_slice_in_dim(conv, h_mine * units, units, 1).reshape(KERNEL, tiles, LANES)
            for conv in (conv_gate, conv_up)
        ],
        axis=2,
    )
    taps = taps.reshape(KERNEL, tiles, 2 * LANES).transpose(1, 0, 2)
    groups = len(weights)
    depth = width // groups
    half_rows = rows // 2
    last = tiles - 1
    gu_spec = pl.BlockSpec((depth, 2 * LANES), lambda i: (0, jnp.minimum(i, last)))
    dn_spec = pl.BlockSpec((depth, units), lambda i: (0, 2))
    out_spec = pl.BlockSpec((half_rows, depth), lambda i: (0, jnp.clip(i - tiles, 0, groups - 1)))
    mine_keep, mine_send, other_keep, other_send = pl.pallas_call(
        functools.partial(ffn_kernel, tiles, groups),
        grid=(tiles + groups,),
        out_shape=[jax.ShapeDtypeStruct((half_rows, width), jnp.bfloat16)] * 4,
        in_specs=[
            SMEM,
            pl.BlockSpec((2, rows, width), lambda i: (0, 0, 0)),
            pl.BlockSpec((2, HALO, width), lambda i: (0, 0, 0)),
            *[gu_spec] * groups,
            *[dn_spec] * groups,
            pl.BlockSpec((1, KERNEL, 2 * LANES), lambda i: (jnp.minimum(i, last), 0, 0)),
        ],
        out_specs=[out_spec] * 4,
        scratch_shapes=[
            pltpu.VMEM((2 * (rows + HALO), width), jnp.bfloat16),
            pltpu.VMEM((2 * rows, units), jnp.bfloat16),
            pltpu.VMEM((2 * (rows + HALO), 2 * LANES), jnp.float32),
        ],
        name="ffn",
    )(mix_table, normed, edge, *weights, *weights, taps)
    far = other_keep.astype(jnp.float32) + over_tp(other_send).astype(jnp.float32)
    far = over_sp(far.astype(jnp.bfloat16), lane_size)
    near = over_tp(mine_send)
    return pl.pallas_call(
        final_kernel,
        out_shape=jax.ShapeDtypeStruct(resid.shape, jnp.bfloat16),
        in_specs=[SMEM, VMEM, VMEM, VMEM, VMEM, VMEM],
        out_specs=VMEM,
        scratch_shapes=[pltpu.VMEM(resid.shape, jnp.float32)],
        name="final",
    )(mix_table, mine_keep, near, far, middle, gain_post[None])


def splits(size):
    return size >= 4 and size & (size - 1) == 0


def split_or_plain(sp_size, tp_size, queries, *rest):
    resid, w_gate = rest[3], rest[7]
    heads = queries.shape[1] // HEAD_DIM
    fits = (
        splits(heads)
        and sp_size % heads == 0
        and resid.shape[1] == sp_size * LANES
        and w_gate.shape[1] % (2 * LANES) == 0
        and queries.shape[0] % (2 * HALO) == 0
    )
    if not fits:
        return plain_local(queries, *rest)
    return split_local(sp_size, tp_size, queries, *rest)


def solution(mesh):
    sp_size, tp_size = mesh.shape["sp"], mesh.shape["tp"]
    in_specs = (
        P("sp", "tp"), P("sp", "tp"), P("sp", "tp"), P("tp"), P(("sp", "tp"), None), P(), P(), P(),
        P("sp", "tp"), P("sp", "tp"), P(None, "tp"), P(None, "tp"), P("tp", "sp"), P(),
    )
    out_specs = P(("sp", "tp"), None)
    local = plain_local
    if tp_size == 2 and splits(sp_size):
        local = functools.partial(split_or_plain, sp_size, tp_size)
    return jax.shard_map(local, mesh=mesh, in_specs=in_specs, out_specs=out_specs, check_vma=False)
```
